32 devices in a mesh: gr: 2 (over x), sp: 8 (over z, y), tp: 2 (over core).
Axes of the slice: x: 2, y: 2, z: 4, core: 2. Of those that a mesh axis runs over, the one named last changes fastest.
Arguments:
- prompt: bfloat16 [2, 2048, 4096], P('gr', 'sp', 'tp'), parts along dimension 0, may hold values from -6 to 6
- key_weight: bfloat16 [4096, 4096], P(None, 'tp'), may hold values from -0.09375 to 0.09375
- value_weight: bfloat16 [4096, 4096], P(None, 'tp'), may hold values from -0.375 to 0.375
- beta_weight: bfloat16 [4096, 32], P(None, 'tp'), may hold values from -0.09375 to 0.09375
- beta_bias: float32 [32], P('tp'), may hold values from -4.5 to -0.5
- decay_rate: float32 [32], P('tp'), may hold values from 0.1 to 3
- new_query: bfloat16 [2, 32, 128], P('gr', 'tp'), parts along dimension 0, may hold values from -6 to 6
- read_gain: float32 [128], replicated, may hold values from 0.1 to 1.9
Outputs:
- state_cache: bfloat16 [2, 32, 128, 128], P('gr', 'tp', 'sp'), parts along dimension 0
- first_read: float32 [2, 32, 128], P('gr', 'tp'), parts along dimension 0
The draws below stay inside these ranges and needn't reach their ends.
There are 2 independent parts, one for each index of `gr`. The reference program is written for one: setup_inputs(seed, part) draws one part's arguments, and reference() takes and returns one part's arrays. A program takes and returns all parts, laid end to end along the dimension named above; an argument that names none is the same for every part. Nothing has to cross between parts.
All inputs are finite; a program needn't handle non-finite values.
Results may differ from the reference program's by a relative error of at most 0.013.
Values may be sent and summed in bfloat16 or wider, within the bound.
A program may use at most 128 MiB of HBM per device.

```python
import math
import jax
import jax.numpy as jnp
from jax import lax

D = 4096
HEADS = 32
HDIM = 128
BLOCK = 64
LEN = 2048


def draw_prompt(key, part):
    shared_key = jax.random.fold_in(key, 11)
    single_key = jax.random.fold_in(key, 12)
    run_count = LEN // BLOCK
    common = 1.5 * jax.random.normal(shared_key, (run_count, 1, D), jnp.float32)
    own_part = 0.75 * jax.random.normal(single_key, (run_count, BLOCK, D), jnp.float32)
    combined = jnp.clip(common + own_part, -6.0, 6.0).reshape(1, LEN, D)
    return combined.astype(jnp.bfloat16)


def level_of(key, extent, split, least, high):
    def one(position, blocks):
        draws = jax.random.uniform(jax.random.fold_in(jax.random.fold_in(key, 6), position), (blocks,), jnp.float32, least / len(split), high / len(split))
        return jnp.repeat(jnp.exp(draws), extent[position] // blocks).reshape((-1,) + (1,) * (len(extent) - position - 1))

    factor_of = one(*split[0])
    for cut in split[1:]:
        factor_of = factor_of * one(*cut)
    return factor_of


def gaussian(own_key, dims, spread, most, split=(), held_as=jnp.bfloat16):
    result = jax.random.normal(own_key, dims, jnp.float32) * spread
    if len(split) > 0:
        result = level_of(own_key, dims, split, -0.22, 0.18) * result
    return jnp.clip(result, min=-most, max=most).astype(held_as)


def setup_inputs(seed: int = 0, part: int = 0) -> dict:
    arg_keys = jax.random.split(jax.random.key(seed), 9)
    own_keys = jax.random.split(jax.random.fold_in(arg_keys[8], part), 9)
    prompt = draw_prompt(jax.random.fold_in(jax.random.fold_in(arg_keys[8], part), 71), part)
    key_weight = gaussian(arg_keys[1], (D, HEADS * HDIM), D ** -0.5, 0.09375, ((1, 2),))
    value_weight = gaussian(arg_keys[2], (D, HEADS * HDIM), (D // 16) ** -0.5, 0.375, ((1, 2),))
    beta_weight = gaussian(arg_keys[3], (D, HEADS), D ** -0.5, 0.09375, ((1, 2),))
    beta_bias = jnp.clip(-4.5 + 4.0 * jax.random.uniform(arg_keys[4], (HEADS,), jnp.float32) ** level_of(arg_keys[4], (HEADS,), ((0, 2),), -0.2, 0.2), -4.5, -0.5)
    decay_rate = jnp.clip(jnp.exp(math.log(3.0) - 3.4011974 * jax.random.uniform(arg_keys[5], (HEADS,), jnp.float32) ** level_of(arg_keys[5], (HEADS,), ((0, 2),), -0.2, 0.2)), 0.1, 3.0)
    new_query = gaussian(own_keys[6], (1, HEADS, HDIM), 1.0, 6.0, ((1, 2),))
    read_gain = jnp.clip(1.0 + 0.18 * jax.random.normal(arg_keys[7], (HDIM,), jnp.float32), 0.1, 1.9)
    return dict(prompt=prompt, key_weight=key_weight, value_weight=value_weight, beta_weight=beta_weight, beta_bias=beta_bias, decay_rate=decay_rate, new_query=new_query, read_gain=read_gain)


def reference(prompt, key_weight, value_weight, beta_weight, beta_bias, decay_rate, new_query, read_gain):
    tokens = prompt[0]
    key_proj = jnp.dot(tokens, key_weight, preferred_element_type=jnp.float32).astype(jnp.bfloat16)
    value_proj = jnp.dot(tokens, value_weight, preferred_element_type=jnp.float32).astype(jnp.bfloat16)
    beta_pre = jnp.dot(tokens, beta_weight, preferred_element_type=jnp.float32)
    key_proj = lax.optimization_barrier(key_proj)
    value_proj = lax.optimization_barrier(value_proj)
    key_rows = key_proj.astype(jnp.float32).reshape(LEN, HEADS, HDIM)
    key_rows = key_rows * lax.rsqrt(lax.optimization_barrier(jnp.sum(key_rows * key_rows, axis=-1, keepdims=True)) + 1.0)
    values = value_proj.astype(jnp.float32).reshape(LEN, HEADS, HDIM)
    strength = jax.nn.sigmoid(beta_pre + beta_bias)
    retain = jnp.exp(-decay_rate / LEN)

    def advance(memory_matrix, inputs):
        single_key_row, value_row, beta_row = inputs
        retrieved_values = jnp.einsum('jg,jgb->jb', single_key_row, memory_matrix, precision=lax.Precision.HIGHEST)
        written_update = beta_row[:, None, None] * single_key_row[:, :, None]
        memory_matrix = retain[:, None, None] * (memory_matrix - written_update * retrieved_values[:, None, :])
        memory_matrix = memory_matrix + written_update * value_row[:, None, :]
        return (memory_matrix, None)
    initial = jnp.zeros((HEADS, HDIM, HDIM), jnp.float32)
    closing_state = lax.scan(advance, initial, (key_rows, values, strength))[0]
    normalized_query = new_query[0].astype(jnp.float32)
    normalized_query = normalized_query * lax.rsqrt(lax.optimization_barrier(jnp.sum(normalized_query * normalized_query, axis=-1, keepdims=True)) + 1.0)
    unscaled_read = jnp.einsum('jg,jgb->jb', normalized_query, closing_state, precision=lax.Precision.HIGHEST)
    read_out = unscaled_read * lax.rsqrt(lax.optimization_barrier(jnp.mean(unscaled_read * unscaled_read, axis=-1, keepdims=True)) + 0.05) * read_gain
    return (closing_state.astype(jnp.bfloat16)[None], read_out[None])
```

```python
import functools

import jax
import jax.numpy as jnp
from jax import lax
from jax.experimental import pallas as pl
from jax.experimental.pallas import tpu as pltpu
from jax.sharding import PartitionSpec as P

MESH = pl.DeviceIdType.MESH
F32 = jnp.float32
BF16 = jnp.bfloat16


def dot(left, right, contract=((1,), (0,))):
    return lax.dot_general(left, right, (contract, ((), ())), preferred_element_type=F32)


def level_masks(size):
    row = lax.broadcasted_iota(jnp.int32, (size, size), 0)
    col = lax.broadcasted_iota(jnp.int32, (size, size), 1)
    masks = []
    for level in range((size - 1).bit_length()):
        together = (row >> (level + 1)) == (col >> (level + 1))
        apart = (row >> level) != (col >> level)
        masks.append((together & apart & (row > col)).astype(F32).astype(BF16))
    return masks


def span(heads, masks, eye):
    keys_t, rights, grams, inverses = [], [], [], []
    for key, value, strength, fade in heads:
        key = key.astype(F32)
        key = key * lax.rsqrt(jnp.sum(key * key, axis=1, keepdims=True) + 1.0)
        weighted = (key * strength).astype(BF16)
        key = key.astype(BF16)
        value = (value.astype(F32) * (strength * fade)).astype(BF16)
        keys_t.append(key)
        rights.append(jnp.concatenate([value, weighted], axis=1))
        grams.append(dot(weighted, key, ((1,), (1,))).astype(BF16))
    for gram in grams:
        inverses.append(eye[...] - gram * masks[0])
    size = grams[0].shape[0]
    levels = (size - 1).bit_length()
    for level in range(1, levels - 1):
        steps = [dot(g * masks[level], x).astype(BF16) for g, x in zip(grams, inverses)]
        inverses = [x - dot(x, s).astype(BF16) for x, s in zip(inverses, steps)]
    half = size // 2
    out = []
    for key, right, gram, x in zip(keys_t, rights, grams, inverses):
        first, last = x[:half, :half], x[half:, half:]
        cross = dot(last, dot(gram[half:, :half], first).astype(BF16)).astype(BF16)
        top, low = key[:half], key[half:]
        y_first = dot(top, first, ((0,), (0,))) - dot(low, cross, ((0,), (0,)))
        y_last = dot(low, last, ((0,), (0,)))
        y = jnp.concatenate([y_first.astype(BF16), y_last.astype(BF16)], axis=1)
        out.append(dot(y, right))
    return out


def kernel(
    n, tp, groups, per, dim,
    prompt, key_w, value_w, beta_w, bias, decay, query, gain,
    state_out, read_out,
    feat, wbuf, mask_buf, eye_buf, strength_buf, send, recv, row_stage, row_recv, read_stage, read_recv,
    feat_send, feat_recv, w_sem, map_send, map_recv, row_send, row_got, read_send, read_got,
):
    me = lax.axis_index("sp")
    core = lax.axis_index("tp")
    seg, part = prompt.shape[1], prompt.shape[2]

    wide = per * dim
    full = seg * n
    stride = n // groups
    everyone = groups == n
    mine = me // stride
    is_owner = lax.rem(me, stride) == 0

    def when_owner(work):
        if everyone:
            work()
        else:
            pl.when(is_owner)(work)

    def group_at(i):
        return lax.rem(mine + 1 + i, groups)

    def fetch(i):
        at = pl.ds(pl.multiple_of(group_at(i) * wide, wide), wide)
        slot = lax.rem(i, 2)
        return [
            pltpu.make_async_copy(w.at[:, at], wbuf.at[slot, j], w_sem.at[slot, j])
            for j, w in enumerate((key_w, value_w))
        ]

    for copy in fetch(0):
        copy.start()

    barrier = pltpu.get_barrier_semaphore()
    for d in range(1, n):
        pl.semaphore_signal(barrier, inc=1, device_id={"sp": lax.rem(me + d, n)}, device_id_type=MESH)
    for d in range(1, tp):
        pl.semaphore_signal(barrier, inc=1, device_id={"tp": lax.rem(core + d, tp)}, device_id_type=MESH)
    pl.semaphore_wait(barrier, n - 1 + tp - 1)

    def feature_copy(d, slot):
        return pltpu.make_async_remote_copy(
            src_ref=prompt.at[0], dst_ref=feat.at[slot],
            send_sem=feat_send.at[d - 1], recv_sem=feat_recv.at[slot],
            device_id={"tp": lax.rem(core + d, tp)}, device_id_type=MESH,
        )

    for d in range(1, tp):
        feature_copy(d, core).start()

    for level, mask in enumerate(level_masks(seg)):
        mask_buf[level] = mask
    ids = [lax.broadcasted_iota(jnp.int32, (seg, seg), axis) for axis in (0, 1)]
    eye_buf[...] = (ids[0] == ids[1]).astype(F32).astype(BF16)

    def project(weights):
        total = dot(prompt[0], weights[pl.ds(pl.multiple_of(core * part, part), part), :])
        for d in range(1, tp):
            other = lax.rem(core + d, tp)
            total += dot(feat[other], weights[pl.ds(pl.multiple_of(other * part, part), part), :])
        return total

    for d in range(1, tp):
        feature_copy(d, lax.rem(core + d, tp)).wait_recv()
    strength_buf[...] = jax.nn.sigmoid(project(beta_w) + bias[...])

    def map_copy(g):
        return pltpu.make_async_remote_copy(
            src_ref=send.at[g], dst_ref=recv.at[me],
            send_sem=map_send.at[g], recv_sem=map_recv.at[me],
            device_id={"sp": g * stride}, device_id_type=MESH,
        )

    def body(i, carry):
        g = group_at(i)
        slot = lax.rem(i, 2)
        for copy in fetch(i):
            copy.wait()

        @pl.when(i + 1 < groups)
        def _():
            for copy in fetch(i + 1):
                copy.start()

        keys = project(wbuf.at[slot, 0]).astype(BF16)
        values = project(wbuf.at[slot, 1]).astype(BF16)

        @pl.when(i > 0)
        def _():
            map_copy(group_at(i - 1)).start()

        strengths = strength_buf[...]
        lane = lax.broadcasted_iota(jnp.int32, strengths.shape, 1)
        rest = full - 1 - me * seg - lax.broadcasted_iota(jnp.int32, (seg, 1), 0)
        rest = rest.astype(F32) * (1.0 / full)
        heads = []
        for h in range(per):
            head = g * per + h
            strength = jnp.sum(jnp.where(lane == head, strengths, 0.0), axis=1, keepdims=True)
            fade = jnp.exp(-decay[head] * rest)
            cols = slice(h * dim, (h + 1) * dim)
            heads.append((keys[:, cols], values[:, cols], strength, fade))
        for h, result in enumerate(span(heads, mask_buf, eye_buf)):
            send[g, h] = result.astype(BF16)
        return carry

    lax.fori_loop(0, groups, body, 0)

    if not everyone:
        @pl.when(jnp.logical_not(is_owner))
        def _():
            map_copy(mine).start()

    rows = dim // n

    def row_copy(q, slot):
        return pltpu.make_async_remote_copy(
            src_ref=row_stage.at[q], dst_ref=row_recv.at[slot],
            send_sem=row_send.at[q], recv_sem=row_got.at[slot],
            device_id={"sp": q}, device_id_type=MESH,
        )

    def read_copy(q, slot):
        return pltpu.make_async_remote_copy(
            src_ref=read_stage, dst_ref=read_recv.at[slot],
            send_sem=read_send.at[q], recv_sem=read_got.at[slot],
            device_id={"sp": q}, device_id_type=MESH,
        )

    def map_arrival(src):
        return pltpu.make_async_remote_copy(
            src_ref=send.at[0], dst_ref=recv.at[src],
            send_sem=map_send.at[0], recv_sem=map_recv.at[src],
            device_id={"sp": me}, device_id_type=MESH,
        )

    def finish():
        recv[me] = send[mine]

        def link(p, states):
            @pl.when(p != me)
            def _():
                map_arrival(p).wait_recv()

            new = []
            for h in range(per):
                write, drop = recv[p, h, :, :dim].astype(F32), recv[p, h, :, dim:]
                high = states[h].astype(BF16)
                low = (states[h] - high.astype(F32)).astype(BF16)
                new.append(states[h] + (write - dot(drop, high) - dot(drop, low)))
            return tuple(new)

        states = lax.fori_loop(0, n, link, tuple(jnp.zeros((dim, dim), F32) for _ in range(per)))
        for h in range(per):
            cast = states[h].astype(BF16)
            for q in range(n):
                row_stage[q, h] = cast[q * rows:(q + 1) * rows]
        unit = query[0].astype(F32)
        unit = unit * lax.rsqrt(jnp.sum(unit * unit, axis=1, keepdims=True) + 1.0)
        which = lax.broadcasted_iota(jnp.int32, unit.shape, 0)
        for h in range(per):
            row = jnp.sum(jnp.where(which == mine * per + h, unit, 0.0), axis=0, keepdims=True)
            raw = jnp.dot(
                jnp.broadcast_to(row, (8, dim)), states[h],
                precision=lax.Precision.HIGHEST, preferred_element_type=F32,
            )[0:1]
            raw = raw * lax.rsqrt(jnp.mean(raw * raw, axis=1, keepdims=True) + 0.05) * gain[...]
            read_stage[h:h + 1] = raw
        for d in range(1, n):
            row_copy(lax.rem(me + d, n), mine).start()
        for d in range(1, n):
            read_copy(lax.rem(me + d, n), mine).start()
        row_recv[mine] = row_stage[me]
        read_recv[mine] = read_stage[...]

    when_owner(finish)

    for g in range(groups):
        @pl.when(me != g * stride)
        def _():
            row_copy(me, g).wait_recv()
            read_copy(me, g).wait_recv()

        for h in range(per):
            state_out[0, g * per + h] = row_recv[g, h]
        read_out[0, g * per:(g + 1) * per] = read_recv[g]

    for d in range(1, tp):
        feature_copy(d, core).wait_send()
    for g in range(groups):
        @pl.when(me != g * stride)
        def _():
            map_copy(g).wait_send()

    def sent():
        for d in range(1, n):
            row_copy(lax.rem(me + d, n), mine).wait_send()
            read_copy(lax.rem(me + d, n), mine).wait_send()

    when_owner(sent)


def solution(mesh):
    n, tp = mesh.shape["sp"], mesh.shape["tp"]

    def shards(prompt, key_w, value_w, beta_w, bias, decay, query, gain):
        seg, part = prompt.shape[1:]
        depth = key_w.shape[0]
        heads = beta_w.shape[1]
        dim = key_w.shape[1] // heads
        per = max(1, heads // n)
        groups = heads // per
        wide = per * dim
        rows = dim // n
        levels = (seg - 1).bit_length()
        dma = pltpu.SemaphoreType.DMA
        vmem = pl.BlockSpec(memory_space=pltpu.VMEM)
        hbm = pl.BlockSpec(memory_space=pl.ANY)
        return pl.pallas_call(
            functools.partial(kernel, n, tp, groups, per, dim),
            out_shape=(
                jax.ShapeDtypeStruct((1, heads, rows, dim), BF16),
                jax.ShapeDtypeStruct((1, heads, dim), F32),
            ),
            in_specs=[vmem, hbm, hbm, vmem, vmem, pl.BlockSpec(memory_space=pltpu.SMEM), vmem, vmem],
            out_specs=(vmem, vmem),
            scratch_shapes=[
                pltpu.VMEM((tp, seg, part), BF16),
                pltpu.VMEM((2, 2, depth, wide), BF16),
                pltpu.VMEM((levels, seg, seg), BF16),
                pltpu.VMEM((seg, seg), BF16),
                pltpu.VMEM((seg, heads), F32),
                pltpu.VMEM((groups, per, dim, 2 * dim), BF16),
                pltpu.VMEM((n, per, dim, 2 * dim), BF16),
                pltpu.VMEM((n, per, rows, dim), BF16),
                pltpu.VMEM((groups, per, rows, dim), BF16),
                pltpu.VMEM((per, dim), F32),
                pltpu.VMEM((groups, per, dim), F32),
                dma((tp - 1,)),
                dma((tp,)),
                dma((2, 2)),
                dma((groups,)),
                dma((n,)),
                dma((n,)),
                dma((groups,)),
                dma((n,)),
                dma((groups,)),
            ],
            compiler_params=pltpu.CompilerParams(
                collective_id=0, has_side_effects=True, vmem_limit_bytes=48 * 2**20
            ),
        )(prompt, key_w, value_w, beta_w, bias.reshape(1, heads), decay, query, gain.reshape(1, dim))

    return jax.shard_map(
        shards,
        mesh=mesh,
        in_specs=(
            P("gr", "sp", "tp"),
            P(None, "tp"),
            P(None, "tp"),
            P(None, "tp"),
            P("tp"),
            P("tp"),
            P("gr", "tp", None),
            P(),
        ),
        out_specs=(P("gr", "tp", "sp", None), P("gr", "tp", None)),
        check_vma=False,
    )
```

```python
import functools

import jax
import jax.numpy as jnp
from jax import lax
from jax.experimental import pallas as pl
from jax.experimental.pallas import tpu as pltpu
from jax.sharding import PartitionSpec as P

MESH = pl.DeviceIdType.MESH
F32 = jnp.float32
BF16 = jnp.bfloat16


def dot(left, right, contract=((1,), (0,))):
    return lax.dot_general(left, right, (contract, ((), ())), preferred_element_type=F32)


def level_masks(size):
    row = lax.broadcasted_iota(jnp.int32, (size, size), 0)
    col = lax.broadcasted_iota(jnp.int32, (size, size), 1)
    masks = []
    for level in range((size - 1).bit_length()):
        together = (row >> (level + 1)) == (col >> (level + 1))
        apart = (row >> level) != (col >> level)
        masks.append((together & apart & (row > col)).astype(F32).astype(BF16))
    return masks


def span(heads, masks, eye):
    keys_t, rights, grams, inverses = [], [], [], []
    for key, value, strength, fade in heads:
        key = key.astype(F32)
        key = key * lax.rsqrt(jnp.sum(key * key, axis=1, keepdims=True) + 1.0)
        weighted = (key * strength).astype(BF16)
        key = key.astype(BF16)
        value = (value.astype(F32) * (strength * fade)).astype(BF16)
        keys_t.append(key)
        rights.append(jnp.concatenate([value, weighted], axis=1))
        grams.append(dot(weighted, key, ((1,), (1,))).astype(BF16))
    for gram in grams:
        inverses.append(eye[...] - gram * masks[0])
    size = grams[0].shape[0]
    levels = (size - 1).bit_length()
    for level in range(1, levels - 1):
        steps = [dot(g * masks[level], x).astype(BF16) for g, x in zip(grams, inverses)]
        inverses = [x - dot(x, s).astype(BF16) for x, s in zip(inverses, steps)]
    half = size // 2
    out = []
    for key, right, gram, x in zip(keys_t, rights, grams, inverses):
        first, last = x[:half, :half], x[half:, half:]
        cross = dot(last, dot(gram[half:, :half], first).astype(BF16)).astype(BF16)
        top, low = key[:half], key[half:]
        y_first = dot(top, first, ((0,), (0,))) - dot(low, cross, ((0,), (0,)))
        y_last = dot(low, last, ((0,), (0,)))
        y = jnp.concatenate([y_first.astype(BF16), y_last.astype(BF16)], axis=1)
        out.append(dot(y, right))
    return out


def kernel(
    n, tp, groups, per, dim, together,
    prompt, key_w, value_w, beta_w, bias, decay, query, gain,
    state_out, read_out,
    feat, first_buf, rest_buf, total, beta_buf, bias_buf, decay_buf, query_buf, gain_buf,
    mask_buf, eye_buf, strength_buf, spans, partner_spans, joined, recv,
    row_stage, row_recv, read_stage, read_recv,
    in_sem, feat_send, feat_recv, first_sem, rest_sem, pair_send, pair_recv,
    map_send, map_recv, row_send, row_got, read_send, read_got,
):
    me = lax.axis_index("sp")
    core = lax.axis_index("tp")
    seg, part = prompt.shape[1], prompt.shape[2]
    wide = per * dim
    full = seg * n
    stride = n // groups
    half = groups // 2
    parity = lax.rem(me, 2)
    mine = me // stride
    slots = first_buf.shape[0]

    def owner(g):
        return g * stride + (lax.rem(g, 2) if stride > 1 else 0)

    is_owner = me == owner(mine)

    def when_owner(work):
        if stride == 1:
            work()
        else:
            pl.when(is_owner)(work)

    def pair_at(j):
        return lax.rem(mine // 2 + 1 + j, half)

    def group_at(index):
        keep = index // half
        return 2 * pair_at(lax.rem(index, half)) + keep * parity + (1 - keep) * (1 - parity)

    def columns(g):
        return pl.ds(pl.multiple_of(g * wide, wide), wide)

    def features_of(d):
        return pl.ds(pl.multiple_of(lax.rem(core + d, tp) * part, part), part)

    def fetch_first(index):
        slot = lax.rem(index, slots)
        return [
            pltpu.make_async_copy(
                w.at[features_of(0), columns(group_at(index))], first_buf.at[slot, j], first_sem.at[slot, j]
            )
            for j, w in enumerate((key_w, value_w))
        ]

    def fetch_rest(step):
        slot = lax.rem(step, 2)
        return [
            pltpu.make_async_copy(
                w.at[features_of(d), columns(group_at(step * together + s))],
                rest_buf.at[slot, s, j, d - 1], rest_sem.at[slot, s, j, d - 1],
            )
            for s in range(together)
            for j, w in enumerate((key_w, value_w))
            for d in range(1, tp)
        ]

    own_prompt = pltpu.make_async_copy(prompt.at[0], feat.at[core], in_sem.at[0])
    small = [
        pltpu.make_async_copy(src, dst, in_sem.at[1 + k])
        for k, (src, dst) in enumerate(
            ((beta_w, beta_buf), (bias, bias_buf), (decay, decay_buf), (query, query_buf), (gain, gain_buf))
        )
    ]
    own_prompt.start()
    for index in range(min(slots - 1, groups)):
        for copy in fetch_first(index):
            copy.start()
    for copy in small:
        copy.start()

    barrier = pltpu.get_barrier_semaphore()
    for d in range(1, n):
        pl.semaphore_signal(barrier, inc=1, device_id={"sp": lax.rem(me + d, n)}, device_id_type=MESH)
    for d in range(1, tp):
        pl.semaphore_signal(barrier, inc=1, device_id={"tp": lax.rem(core + d, tp)}, device_id_type=MESH)
    own_prompt.wait()
    pl.semaphore_wait(barrier, n - 1 + tp - 1)

    def feature_copy(d, slot):
        return pltpu.make_async_remote_copy(
            src_ref=feat.at[core], dst_ref=feat.at[slot],
            send_sem=feat_send.at[d - 1], recv_sem=feat_recv.at[slot],
            device_id={"tp": lax.rem(core + d, tp)}, device_id_type=MESH,
        )

    for d in range(1, tp):
        feature_copy(d, core).start()

    def project_first(index, carry):
        @pl.when(index + slots - 1 < groups)
        def _():
            for copy in fetch_first(index + slots - 1):
                copy.start()

        for copy in fetch_first(index):
            copy.wait()
        slot, g = lax.rem(index, slots), group_at(index)
        for j in range(2):
            total[g, j] = dot(feat[core], first_buf[slot, j])
        return carry

    lax.fori_loop(0, groups, project_first, 0)
    for copy in fetch_rest(0):
        copy.start()

    for level, mask in enumerate(level_masks(seg)):
        mask_buf[level] = mask
    ids = [lax.broadcasted_iota(jnp.int32, (seg, seg), axis) for axis in (0, 1)]
    eye_buf[...] = (ids[0] == ids[1]).astype(F32).astype(BF16)
    for copy in small:
        copy.wait()
    before = dot(feat[core], beta_buf[:, features_of(0)], ((1,), (1,)))
    for d in range(1, tp):
        other = lax.rem(core + d, tp)
        feature_copy(d, other).wait_recv()
        before += dot(feat[other], beta_buf[:, features_of(d)], ((1,), (1,)))
    strength_buf[...] = jax.nn.sigmoid(before + bias_buf[...])

    def pair_copy(m):
        return pltpu.make_async_remote_copy(
            src_ref=spans.at[0, m], dst_ref=partner_spans.at[m],
            send_sem=pair_send.at[m], recv_sem=pair_recv.at[m],
            device_id={"sp": me + 1 - 2 * parity}, device_id_type=MESH,
        )

    def map_copy(m, slot):
        return pltpu.make_async_remote_copy(
            src_ref=joined.at[m], dst_ref=recv.at[slot],
            send_sem=map_send.at[m], recv_sem=map_recv.at[slot],
            device_id={"sp": owner(2 * m + parity)}, device_id_type=MESH,
        )

    def send(step):
        for s in range(together):
            index = step * together + s
            m = pair_at(lax.rem(index, half))

            @pl.when(index < half)
            def _():
                pair_copy(m).start()

            @pl.when((index >= half) & (owner(2 * m + parity) != me))
            def _():
                map_copy(m, me // 2).start()

    def body(step, carry):
        slot = lax.rem(step, 2)

        @pl.when(step + 1 < groups // together)
        def _():
            for copy in fetch_rest(step + 1):
                copy.start()

        for copy in fetch_rest(step):
            copy.wait()
        projected = []
        for s in range(together):
            g = group_at(step * together + s)
            pair = []
            for j in range(2):
                acc = total[g, j]
                for d in range(1, tp):
                    acc += dot(feat[lax.rem(core + d, tp)], rest_buf[slot, s, j, d - 1])
                pair.append(acc.astype(BF16))
            projected.append(pair)

        @pl.when(step > 0)
        def _():
            send(step - 1)

        strengths = strength_buf[...]
        rates = decay_buf[...]
        lane = lax.broadcasted_iota(jnp.int32, strengths.shape, 1)
        rest = full - 1 - me * seg - lax.broadcasted_iota(jnp.int32, (seg, 1), 0)
        rest = rest.astype(F32) * (1.0 / full)
        heads = []
        for s in range(together):
            g = group_at(step * together + s)
            keys, values = projected[s]
            for h in range(per):
                head = g * per + h
                strength = jnp.sum(jnp.where(lane == head, strengths, 0.0), axis=1, keepdims=True)
                rate = jnp.sum(jnp.where(lane[:1] == head, rates, 0.0), axis=1, keepdims=True)
                fade = jnp.exp(-rate * rest)
                cols = slice(h * dim, (h + 1) * dim)
                heads.append((keys[:, cols], values[:, cols], strength, fade))
        keep = step * together // half
        for k, result in enumerate(span(heads, mask_buf, eye_buf)):
            m = pair_at(lax.rem(step * together + k // per, half))
            spans[keep, m, k % per] = result.astype(BF16)

        @pl.when(keep == 1)
        def _():
            for s in range(together):
                m = pair_at(lax.rem(step * together + s, half))
                pair_copy(m).wait_recv()
                for h in range(per):
                    ours, theirs = spans[1, m, h], partner_spans[m, h]
                    early = jnp.where(parity == 1, theirs, ours)
                    late = jnp.where(parity == 1, ours, theirs)
                    both = early.astype(F32) + late.astype(F32) - dot(late[:, dim:], early)
                    joined[m, h] = both.astype(BF16)

        return carry

    lax.fori_loop(0, groups // together, body, 0)
    recv[me // 2] = joined[mine // 2]
    send(groups // together - 1)

    rows = dim // n

    def row_copy(q, slot):
        return pltpu.make_async_remote_copy(
            src_ref=row_stage.at[q], dst_ref=row_recv.at[slot],
            send_sem=row_send.at[q], recv_sem=row_got.at[slot],
            device_id={"sp": q}, device_id_type=MESH,
        )

    def read_copy(q, slot):
        return pltpu.make_async_remote_copy(
            src_ref=read_stage, dst_ref=read_recv.at[slot],
            send_sem=read_send.at[q], recv_sem=read_got.at[slot],
            device_id={"sp": q}, device_id_type=MESH,
        )

    def finish():
        def link(p, states):
            @pl.when(p != me // 2)
            def _():
                map_copy(0, p).wait_recv()

            new = []
            for h in range(per):
                write, drop = recv[p, h, :, :dim].astype(F32), recv[p, h, :, dim:]
                high = states[h].astype(BF16)
                low = (states[h] - high.astype(F32)).astype(BF16)
                new.append(states[h] + (write - dot(drop, high) - dot(drop, low)))
            return tuple(new)

        states = lax.fori_loop(0, n // 2, link, tuple(jnp.zeros((dim, dim), F32) for _ in range(per)))
        for h in range(per):
            cast = states[h].astype(BF16)
            for q in range(n):
                row_stage[q, h] = cast[q * rows:(q + 1) * rows]
        unit = query_buf[0].astype(F32)
        unit = unit * lax.rsqrt(jnp.sum(unit * unit, axis=1, keepdims=True) + 1.0)
        which = lax.broadcasted_iota(jnp.int32, unit.shape, 0)
        for h in range(per):
            row = jnp.sum(jnp.where(which == mine * per + h, unit, 0.0), axis=0, keepdims=True)
            raw = jnp.dot(
                jnp.broadcast_to(row, (8, dim)), states[h],
                precision=lax.Precision.HIGHEST, preferred_element_type=F32,
            )[0:1]
            raw = raw * lax.rsqrt(jnp.mean(raw * raw, axis=1, keepdims=True) + 0.05) * gain_buf[...]
            read_stage[h:h + 1] = raw
        for d in range(1, n):
            row_copy(lax.rem(me + d, n), mine).start()
        for d in range(1, n):
            read_copy(lax.rem(me + d, n), mine).start()
        row_recv[mine] = row_stage[me]
        read_recv[mine] = read_stage[...]

    when_owner(finish)

    for g in range(groups):
        @pl.when(me != owner(g))
        def _():
            row_copy(me, g).wait_recv()
            read_copy(me, g).wait_recv()

        for h in range(per):
            state_out[0, g * per + h] = row_recv[g, h]
        read_out[0, g * per:(g + 1) * per] = read_recv[g]

    for d in range(1, tp):
        feature_copy(d, core).wait_send()
    for m in range(half):
        pair_copy(m).wait_send()

        @pl.when(owner(2 * m + parity) != me)
        def _():
            map_copy(m, 0).wait_send()

    def sent():
        for d in range(1, n):
            row_copy(lax.rem(me + d, n), mine).wait_send()
            read_copy(lax.rem(me + d, n), mine).wait_send()

    when_owner(sent)


def solution(mesh):
    n, tp = mesh.shape["sp"], mesh.shape["tp"]

    def shards(prompt, key_w, value_w, beta_w, bias, decay, query, gain):
        seg, part = prompt.shape[1:]
        depth = key_w.shape[0]
        heads = beta_w.shape[1]
        dim = key_w.shape[1] // heads
        per = max(1, heads // n)
        groups = heads // per
        wide = per * dim
        rows = dim // n
        levels = (seg - 1).bit_length()
        dma = pltpu.SemaphoreType.DMA
        vmem = pl.BlockSpec(memory_space=pltpu.VMEM)
        hbm = pl.BlockSpec(memory_space=pl.ANY)
        half = groups // 2
        together = min(2, half)
        slots = 4
        return pl.pallas_call(
            functools.partial(kernel, n, tp, groups, per, dim, together),
            out_shape=(
                jax.ShapeDtypeStruct((1, heads, rows, dim), BF16),
                jax.ShapeDtypeStruct((1, heads, dim), F32),
            ),
            in_specs=[hbm] * 8,
            out_specs=(vmem, vmem),
            scratch_shapes=[
                pltpu.VMEM((tp, seg, part), BF16),
                pltpu.VMEM((slots, 2, part, wide), BF16),
                pltpu.VMEM((2, together, 2, tp - 1, part, wide), BF16),
                pltpu.VMEM((groups, 2, seg, wide), F32),
                pltpu.VMEM((heads, depth), BF16),
                pltpu.VMEM((1, heads), F32),
                pltpu.VMEM((1, heads), F32),
                pltpu.VMEM((1, heads, dim), BF16),
                pltpu.VMEM((1, dim), F32),
                pltpu.VMEM((levels, seg, seg), BF16),
                pltpu.VMEM((seg, seg), BF16),
                pltpu.VMEM((seg, heads), F32),
                pltpu.VMEM((2, half, per, dim, 2 * dim), BF16),
                pltpu.VMEM((half, per, dim, 2 * dim), BF16),
                pltpu.VMEM((half, per, dim, 2 * dim), BF16),
                pltpu.VMEM((n // 2, per, dim, 2 * dim), BF16),
                pltpu.VMEM((n, per, rows, dim), BF16),
                pltpu.VMEM((groups, per, rows, dim), BF16),
                pltpu.VMEM((per, dim), F32),
                pltpu.VMEM((groups, per, dim), F32),
                dma((6,)),
                dma((tp - 1,)),
                dma((tp,)),
                dma((slots, 2)),
                dma((2, together, 2, tp - 1)),
                dma((half,)),
                dma((half,)),
                dma((half,)),
                dma((n // 2,)),
                dma((n,)),
                dma((groups,)),
                dma((n,)),
                dma((groups,)),
            ],
            compiler_params=pltpu.CompilerParams(
                collective_id=0, has_side_effects=True, vmem_limit_bytes=60 * 2**20
            ),
        )(
            prompt, key_w, value_w, beta_w.T, bias.reshape(1, heads), decay.reshape(1, heads),
            query, gain.reshape(1, dim),
        )

    return jax.shard_map(
        shards,
        mesh=mesh,
        in_specs=(
            P("gr", "sp", "tp"),
            P(None, "tp"),
            P(None, "tp"),
            P(None, "tp"),
            P("tp"),
            P("tp"),
            P("gr", "tp", None),
            P(),
        ),
        out_specs=(P("gr", "tp", "sp", None), P("gr", "tp", None)),
        check_vma=False,
    )
```
